32 devices in a mesh: sp: 8 (over z, core), tp: 4 (over y, x).
Axes of the slice: x: 2, y: 2, z: 4, core: 2. Of those that a mesh axis runs over, the one named last changes fastest.
Arguments:
- residual: bfloat16 [3072, 2048], P('sp', 'tp'), may hold values from -40 to 40
- norm_gain: bfloat16 [3, 2048], P(None, 'tp'), may hold values from 0.099609375 to 1.8984375
- w_query: bfloat16 [3, 2048, 2048], P(None, 'tp'), may hold values from -2 to 2
- w_key: bfloat16 [3, 2048, 2048], P(None, 'tp'), may hold values from -8 to 8
- w_value: bfloat16 [3, 2048, 2048], P(None, 'tp'), may hold values from -0.125 to 0.125
- w_out: bfloat16 [3, 2048, 2048], P(None, 'tp'), may hold values from -0.25 to 0.25
- offset_bias: float32 [3, 32, 15, 31], P(None, 'tp'), may hold values from -5 to 5
Outputs:
- out_residual: bfloat16 [3072, 2048], P('sp', 'tp')
The draws below stay inside these ranges and needn't reach their ends.
All inputs are finite; a program needn't handle non-finite values.
Results may differ from the reference program's by a relative error of at most 0.014.
Values may be sent and summed in bfloat16 or wider, within the bound.
No kernel may reach another device: no remote copies, remote signals or barrier semaphores. Data moves between devices by JAX's collectives and lax.ppermute only.
A program may use at most 128 MiB of HBM per device.

```python
import math
import jax
import jax.numpy as jnp
from jax import lax

D = 2048
HEADS = 32
HEAD_DIM = 64
GRID_W = 64
NA_ROWS = 8
NA_COLS = 16
LAYERS = 3
NA_W = 2048
ROWS = 48
TOKENS = 3072


def draw_residual(key, part):
    key_one, key_two = jax.random.split(jax.random.fold_in(key, 3), 2)
    ramp = jnp.arange(D, dtype=jnp.float32) / max(D - 1, 1)
    col_scale = jnp.exp(math.log(6.0) * ramp) / 2.5 * jnp.exp(jax.random.uniform(key_two, (D,), jnp.float32, -0.7, 0.7))
    values = jnp.clip(jax.random.normal(key_one, (TOKENS, D), jnp.float32), -4.0, 4.0)
    result = values * col_scale
    return result.astype(jnp.bfloat16)


def query_key_pair(key):
    key_query, key_key = jax.random.split(jax.random.fold_in(key, 11), 2)
    std = D ** (-0.5)
    query_w = jnp.clip(jax.random.normal(key_query, (LAYERS, NA_W, D), jnp.float32), -5.0, 5.0) * std
    key_w = jnp.clip(jax.random.normal(key_key, (LAYERS, NA_W, D), jnp.float32), -5.0, 5.0) * std
    return (query_w, key_w)


def draw_w_query(key, part):
    return query_key_pair(key)[0].astype(jnp.bfloat16)


def draw_w_key(key, part):
    return query_key_pair(key)[1].astype(jnp.bfloat16)


def block_scale(rng, extent, shards, smallest, largest):
    gain = 1.0
    for axis_at, parts in shards:
        draws = jax.random.uniform(jax.random.fold_in(jax.random.fold_in(rng, 6), axis_at), (parts,), jnp.float32, smallest / len(shards), largest / len(shards))
        gain = gain * jnp.repeat(jnp.exp(draws), extent[axis_at] // parts).reshape((-1,) + (1,) * (len(extent) - 1 - axis_at))
    return gain


def gaussian(rng, shape, scale, limit, shards=(), kind=jnp.bfloat16):
    drawn = jax.random.normal(rng, shape, jnp.float32) * scale
    if len(shards) > 0:
        drawn = block_scale(rng, shape, shards, -0.22, 0.18) * drawn
    return jnp.clip(drawn, min=-limit, max=limit).astype(kind)


def setup_inputs(seed: int = 0) -> dict:
    seeds = jax.random.split(jax.random.key(seed), 8)
    return {
        "residual": draw_residual(jax.random.fold_in(seeds[7], 71), 0),
        "norm_gain": jnp.clip(1.0 + 0.18 * jax.random.normal(seeds[1], (LAYERS, D), jnp.float32), 0.099609375, 1.8984375).astype(jnp.bfloat16),
        "w_query": draw_w_query(jax.random.fold_in(seeds[7], 71), 0),
        "w_key": draw_w_key(jax.random.fold_in(seeds[7], 71), 0),
        "w_value": gaussian(seeds[4], (LAYERS, NA_W, D), D ** -0.5, 0.125, ((1, 4),)),
        "w_out": gaussian(seeds[5], (LAYERS, D, NA_W), (NA_W // 4) ** -0.5, 0.25, ((1, 4),)),
        "offset_bias": gaussian(seeds[6], (LAYERS, HEADS, 2 * NA_ROWS - 1, 2 * NA_COLS - 1), 1.0, 5.0, ((1, 4),), jnp.float32),
    }


epsilon = 1e-06

def attend(queries, keys, values, lookup):
    rows_all = ROWS
    query_grid = queries.reshape(rows_all, GRID_W, HEADS, HEAD_DIM)
    key_grid = keys.reshape(rows_all, GRID_W, HEADS, HEAD_DIM)
    value_grid = values.reshape(rows_all, GRID_W, HEADS, HEAD_DIM)
    columns = jnp.arange(GRID_W, dtype=jnp.int32)
    col_index = jnp.clip(columns - NA_COLS // 2, 0, GRID_W - NA_COLS)[:, None] + jnp.arange(NA_COLS, dtype=jnp.int32)
    col_offset = col_index - columns[:, None] + (NA_COLS - 1)

    def row_block(row_global):
        first_row = jnp.clip(row_global - NA_ROWS // 2, 0, rows_all - NA_ROWS).astype(jnp.int32)
        query_row = lax.dynamic_index_in_dim(query_grid, row_global, 0, keepdims=False).astype(jnp.float32)
        key_window = lax.dynamic_slice_in_dim(key_grid, first_row, NA_ROWS, 0)[:, col_index].astype(jnp.float32)
        value_window = lax.dynamic_slice_in_dim(value_grid, first_row, NA_ROWS, 0)[:, col_index].astype(jnp.float32)
        row_offset = first_row + jnp.arange(NA_ROWS, dtype=jnp.int32) - row_global + (NA_ROWS - 1)
        bias_terms = lookup[:, row_offset[:, None, None], col_offset[None, :, :]].transpose(0, 2, 1, 3)
        scores = jnp.einsum('whd,rwkhd->hwrk', query_row, key_window) * HEAD_DIM ** (-0.5) + bias_terms
        weights = jax.nn.softmax(scores.reshape(HEADS, GRID_W, NA_ROWS * NA_COLS), axis=-1).astype(jnp.bfloat16)
        weights = lax.optimization_barrier(weights).astype(jnp.float32).reshape(HEADS, GRID_W, NA_ROWS, NA_COLS)
        attended = jnp.einsum('hwrk,rwkhd->whd', weights, value_window)
        return attended.astype(jnp.bfloat16).reshape(GRID_W, NA_W)
    return lax.map(row_block, jnp.arange(rows_all, dtype=jnp.int32)).reshape(rows_all * GRID_W, NA_W)

def reference(residual, norm_gain, w_query, w_key, w_value, w_out, offset_bias):
    stream = residual
    for layer_index in range(LAYERS):
        res_float = stream.astype(jnp.float32)
        mean_square = lax.optimization_barrier(jnp.mean(res_float * res_float, axis=1, keepdims=True))
        normed = (res_float * lax.rsqrt(mean_square + epsilon) * norm_gain[layer_index].astype(jnp.float32)).astype(jnp.bfloat16)
        queries = jnp.dot(normed, w_query[layer_index].T, preferred_element_type=jnp.float32).astype(jnp.bfloat16)
        keys = jnp.dot(normed, w_key[layer_index].T, preferred_element_type=jnp.float32).astype(jnp.bfloat16)
        values = jnp.dot(normed, w_value[layer_index].T, preferred_element_type=jnp.float32).astype(jnp.bfloat16)
        queries, keys, values = lax.optimization_barrier((queries, keys, values))
        attended = attend(queries, keys, values, offset_bias[layer_index])
        mixed = jnp.dot(attended, w_out[layer_index].T, preferred_element_type=jnp.float32)
        stream = (res_float + mixed).astype(jnp.bfloat16)
    return stream
```

```python
import functools

import jax
import jax.numpy as jnp
from jax import lax
from jax.experimental import pallas as pl
from jax.experimental.pallas import tpu as pltpu
from jax.sharding import PartitionSpec as P

HEAD_DIM = 64
GRID_W = 64
NA_ROWS = 8
NA_COLS = 16
LAYERS = 3
REACH = NA_ROWS // 2
LANES = 128
DIRECT = False
MASKED = -1e30

epsilon = 1e-06


SMEM = pl.BlockSpec(memory_space=pltpu.SMEM)
VMEM = pl.BlockSpec(memory_space=pltpu.VMEM)
PARAMS = pltpu.CompilerParams(vmem_limit_bytes=16 * 1024 * 1024)
ANY = pl.BlockSpec(memory_space=pl.ANY)


def contract(left, right):
    return lax.dot_general(
        left, right, (((1,), (1,)), ((), ())), preferred_element_type=jnp.float32
    )


def weight_copies(src, weight, layer, scratch, sems, width, which):
    return [
        pltpu.make_async_copy(
            weight.at[layer, :, pl.ds(pl.multiple_of(src[k] * width, width), width)],
            scratch.at[:, pl.ds(at * width, width)],
            sems.at[at],
        )
        for at, k in enumerate(which)
    ]


def piece_value(refs):
    parts = [ref[...] for ref in refs]
    return parts[0] if len(parts) == 1 else jnp.concatenate(parts, axis=0)


def grouped(refs, counts):
    groups, at = [], 0
    for count in counts:
        groups.append(refs[at : at + count])
        at += count
    return groups


def start_all(copies):
    for copy in copies:
        copy.start()


def wait_all(copies):
    for copy in copies:
        copy.wait()


def gained_pieces(pieces, gains, layer, gained, width):
    squares = 0.0
    for at, refs_k in enumerate(pieces):
        value = piece_value(refs_k).astype(jnp.float32)
        squares = squares + jnp.sum(value * value, axis=1, keepdims=True)
        gain = gains[at][layer : layer + 1, :].astype(jnp.float32)
        gained[:, at * width : (at + 1) * width] = (value * gain).astype(jnp.bfloat16)
    return squares


def early_kv_kernel(layer, counts, width, which, src, *refs):
    total = sum(counts)
    pieces = grouped(refs[:total], counts)
    gains = refs[total : total + len(counts)]
    wk, wv, keys, values, squares, gained, key_w, value_w, sems = refs[total + len(counts) :]
    key_copies = weight_copies(src, wk, layer, key_w, sems.at[0], width, which)
    value_copies = weight_copies(src, wv, layer, value_w, sems.at[1], width, which)
    start_all(key_copies + value_copies)
    found = gained_pieces(pieces, gains, layer, gained, width)
    squares[...] = jnp.broadcast_to(found, squares.shape)
    wait_all(key_copies)
    keys[...] = contract(gained[...], key_w[...])
    wait_all(value_copies)
    values[...] = contract(gained[...], value_w[...])


def late_kv_kernel(layer, counts, width, which, src, *refs, group, feats, early):
    total = sum(counts)
    pieces = grouped(refs[:total], counts)
    gains = refs[total : total + len(counts)]
    rest = refs[total + len(counts) :]
    wk, wv = rest[:2]
    sums = rest[2:5] if early else (None, None, None)
    kv, head, tail, inverse, gained, key_w, value_w, sems = rest[5 if early else 2 :]
    key_copies = weight_copies(src, wk, layer, key_w, sems.at[0], width, which)
    value_copies = weight_copies(src, wv, layer, value_w, sems.at[1], width, which)
    start_all(key_copies + value_copies)
    squares = gained_pieces(pieces, gains, layer, gained, width)
    if early:
        squares = squares + sums[2][:, :1]
    scale = lax.rsqrt(squares / feats + epsilon)
    inverse[...] = jnp.broadcast_to(scale, inverse.shape)
    for kind, (copies, scratch) in enumerate(((key_copies, key_w), (value_copies, value_w))):
        wait_all(copies)
        result = contract(gained[...], scratch[...])
        if early:
            result = result + sums[kind][...]
        result = (result * scale).astype(jnp.bfloat16)
        for p in range(scratch.shape[0] // group):
            at = (2 * p + kind) * group
            kv[:, at : at + group] = result[:, p * group : (p + 1) * group]
    size = head.shape[0]
    head[...] = kv[:size, :]
    tail[...] = kv[kv.shape[0] - size :, :]


def query_kernel(layer, counts, width, which, src, *refs):
    total = sum(counts)
    pieces = grouped(refs[:total], counts)
    gains = refs[total : total + len(counts)]
    wq, inverse, out, gained, scratch, sems = refs[total + len(counts) :]
    copies = weight_copies(src, wq, layer, scratch, sems, width, which)
    start_all(copies)
    gained_pieces(pieces, gains, layer, gained, width)
    wait_all(copies)
    result = contract(gained[...], scratch[...]) * inverse[:, :1]
    out[...] = (result.astype(jnp.bfloat16) * HEAD_DIM ** (-0.5)).astype(jnp.bfloat16)


def out_kernel(layer, counts, width, which, src, *refs):
    total = sum(counts)
    pieces = grouped(refs[:total], counts)
    wo, *bases = refs[total : len(refs) - 4]
    out, att, scratch, sems = refs[-4:]
    copies = weight_copies(src, wo, layer, scratch, sems, width, which)
    start_all(copies)
    for k, refs_k in enumerate(pieces):
        att[:, k * width : (k + 1) * width] = piece_value(refs_k)
    wait_all(copies)
    mixed = contract(att[...], scratch[...])
    for base in bases:
        mixed = mixed + base[...].astype(jnp.float32)
    out[...] = mixed.astype(out.dtype)


def attend_kernel(rows, group, meta, base, query, *refs):
    parts, (out, keys, values, table) = refs[:-4], refs[-4:]
    at = 0
    for part in parts:
        size = part.shape[0]
        keys[at : at + size, :] = part[:, :group]
        values[at : at + size, :] = part[:, group:]
        at += size
    key_col = lax.broadcasted_iota(jnp.int32, (GRID_W, LANES), 0)
    query_col = lax.broadcasted_iota(jnp.int32, (GRID_W, LANES), 1) % GRID_W
    first_col = jnp.clip(query_col - NA_COLS // 2, 0, GRID_W - NA_COLS)
    inside = (key_col >= first_col) & (key_col < first_col + NA_COLS)
    for d in range(2 * NA_ROWS - 1):
        line = jnp.broadcast_to(base[0, d : d + 1, :], (GRID_W, LANES))
        shifted = pltpu.roll(line, 0, 1, stride=1, stride_axis=0)
        shifted = jnp.where(inside, shifted, MASKED)
        table[d * GRID_W : (d + 1) * GRID_W, :] = shifted[:, :group]
    heads = group // HEAD_DIM
    lane_head = lax.broadcasted_iota(jnp.int32, (GRID_W, group), 1) // HEAD_DIM
    span = NA_ROWS * GRID_W
    for i in range(rows):
        first = pl.multiple_of(meta[0, i] * GRID_W, GRID_W)
        offset = pl.multiple_of(meta[1, i] * GRID_W, GRID_W)
        query_row = query[i * GRID_W : (i + 1) * GRID_W, :]
        spread = jnp.concatenate(
            [jnp.where(lane_head == h, query_row, jnp.zeros_like(query_row)) for h in range(heads)],
            axis=0,
        )
        scores = contract(keys[pl.ds(first, span), :], spread) + table[pl.ds(offset, span), :]
        largest = jnp.max(scores, axis=0, keepdims=True)
        raised = jnp.exp(scores - largest)
        weights = (raised * (1.0 / jnp.sum(raised, axis=0, keepdims=True))).astype(jnp.bfloat16)
        mixed = lax.dot_general(
            weights,
            values[pl.ds(first, span), :],
            (((0,), (0,)), ((), ())),
            preferred_element_type=jnp.float32,
        )
        picked = mixed[:GRID_W]
        for h in range(1, heads):
            picked = jnp.where(lane_head == h, mixed[h * GRID_W : (h + 1) * GRID_W], picked)
        out[i * GRID_W : (i + 1) * GRID_W, :] = picked.astype(jnp.bfloat16)


def exchange(array, bit):
    size = lax.axis_size("tp")
    return lax.ppermute(array, "tp", [(i, i ^ bit) for i in range(size)])


def gather_pieces(array, split=not DIRECT):
    if lax.axis_size("tp") != 4:
        return [[lax.all_gather(array, "tp", axis=1, tiled=True)]]
    one, two = exchange(array, 1), exchange(array, 2)
    if not split:
        return [[array], [one], [two], [exchange(array, 3)]]
    half = array.shape[0] // 2
    return [[array], [one], [two], [exchange(one[:half], 2), exchange(two[half:], 1)]]


def bias_lines(offset_bias, heads):
    layers, count = offset_bias.shape[:2]
    turned = offset_bias[..., ::-1].reshape(layers, count // heads, heads, *offset_bias.shape[2:])
    reach = NA_COLS - 1
    wide = turned.shape[-1]
    head_zero = turned[:, :, 0]
    gap = GRID_W - wide
    zeros = functools.partial(jnp.zeros, dtype=offset_bias.dtype)
    pieces = [head_zero[..., reach:], zeros(head_zero.shape[:-1] + (gap,))]
    for h in range(1, LANES // GRID_W):
        pieces.append(turned[:, :, h] if h < heads else zeros(head_zero.shape))
        pieces.append(zeros(head_zero.shape[:-1] + (gap,)))
    pieces.append(head_zero[..., :reach])
    return jnp.concatenate(pieces, axis=-1)


def per_device(residual, norm_gain, w_query, w_key, w_value, w_out, offset_bias):
    token_count, local_feats = residual.shape
    local_heads = offset_bias.shape[1]
    head_cols = local_heads * HEAD_DIM
    feats = w_query.shape[2]
    heads = LANES // HEAD_DIM if local_heads % (LANES // HEAD_DIM) == 0 else 1
    group = heads * HEAD_DIM
    groups = local_heads // heads
    rows_dev = token_count // GRID_W
    sp_size = lax.axis_size("sp")
    rows_all = rows_dev * sp_size
    row_base = lax.axis_index("sp") * rows_dev
    up = [(i, i + 1) for i in range(sp_size - 1)]
    down = [(j, i) for i, j in up]

    row_global = row_base + jnp.arange(rows_dev, dtype=jnp.int32)
    first_row = jnp.clip(row_global - REACH, 0, rows_all - NA_ROWS)
    meta = jnp.stack([first_row - row_base + REACH, first_row - row_global + NA_ROWS - 1])
    lines = bias_lines(offset_bias, heads)

    gain_pieces = [piece[0] for piece in gather_pieces(norm_gain, split=False)]
    parts_count = len(gain_pieces)
    width = feats // parts_count
    order = jnp.arange(parts_count, dtype=jnp.int32)
    src = order ^ lax.axis_index("tp").astype(jnp.int32) if parts_count > 1 else order

    every = tuple(range(parts_count))
    early, late = every[:-1], every[-1:]
    f32, bf16 = jnp.float32, jnp.bfloat16
    halo = REACH * GRID_W

    def shape(rows, cols, kind=bf16):
        return jax.ShapeDtypeStruct((rows, cols), kind)

    def scratch(rows, which):
        return pltpu.VMEM((rows, len(which) * width), bf16)

    def sems(*dims):
        return pltpu.SemaphoreType.DMA(dims)

    def call(kernel, name, layer, which, pieces, operands, spaces, outs, scratches, **extra):
        chosen = [pieces[k] for k in which]
        flat = [part for piece in chosen for part in piece]
        counts = tuple(len(piece) for piece in chosen)
        return pl.pallas_call(
            functools.partial(kernel, layer, counts, width, which, **extra),
            out_shape=outs,
            in_specs=[SMEM] + [VMEM] * len(flat) + spaces,
            out_specs=jax.tree.map(lambda _: VMEM, outs),
            scratch_shapes=scratches,
            compiler_params=PARAMS,
            name=f"{name}_{layer}",
        )(src, *flat, *operands)

    stream = residual
    for layer in range(LAYERS):
        pieces = gather_pieces(stream)
        sums = ()
        if early:
            sums = call(
                early_kv_kernel, "early_kv", layer, early, pieces,
                [gain_pieces[k] for k in early] + [w_key, w_value],
                [VMEM] * len(early) + [ANY, ANY],
                (
                    shape(token_count, head_cols, f32),
                    shape(token_count, head_cols, f32),
                    shape(token_count, LANES, f32),
                ),
                [scratch(token_count, early)] + [scratch(head_cols, early)] * 2 + [sems(2, len(early))],
            )
        kv, head, tail, inverse = call(
            late_kv_kernel, "late_kv", layer, late, pieces,
            [gain_pieces[k] for k in late] + [w_key, w_value, *sums],
            [VMEM] * len(late) + [ANY, ANY] + [VMEM] * len(sums),
            (
                shape(token_count, 2 * head_cols),
                shape(halo, 2 * head_cols),
                shape(halo, 2 * head_cols),
                shape(token_count, LANES, f32),
            ),
            [scratch(token_count, late)] + [scratch(head_cols, late)] * 2 + [sems(2, len(late))],
            group=group, feats=feats, early=bool(early),
        )
        after = lax.ppermute(head, "sp", down)
        before = lax.ppermute(tail, "sp", up)
        queries = call(
            query_kernel, "query", layer, every, pieces,
            gain_pieces + [w_query, inverse],
            [VMEM] * parts_count + [ANY, VMEM],
            shape(token_count, head_cols),
            [scratch(token_count, every), scratch(head_cols, every), sems(parts_count)],
        )
        window = [before, kv, after]
        reach_tokens = sum(part.shape[0] for part in window)
        attended = pl.pallas_call(
            functools.partial(attend_kernel, rows_dev, group),
            grid=(groups,),
            out_shape=shape(token_count, head_cols),
            in_specs=[
                SMEM,
                pl.BlockSpec((1,) + lines.shape[2:], lambda p: (p, 0, 0)),
                pl.BlockSpec((token_count, group), lambda p: (0, p)),
            ]
            + [pl.BlockSpec((part.shape[0], 2 * group), lambda p: (0, p)) for part in window],
            out_specs=pl.BlockSpec((token_count, group), lambda p: (0, p)),
            scratch_shapes=[
                pltpu.VMEM((reach_tokens, group), bf16),
                pltpu.VMEM((reach_tokens, group), bf16),
                pltpu.VMEM(((2 * NA_ROWS - 1) * GRID_W, group), f32),
            ],
            compiler_params=PARAMS,
            name=f"attend_{layer}",
        )(meta, lines[layer], queries, *window)
        pieces = gather_pieces(attended)
        bases = [stream]
        if early:
            bases.append(
                call(
                    out_kernel, "early_out", layer, early, pieces, [w_out], [ANY],
                    shape(token_count, local_feats, f32),
                    [scratch(token_count, early), scratch(local_feats, early), sems(len(early))],
                )
            )
        stream = call(
            out_kernel, "late_out", layer, late, pieces, [w_out, *bases],
            [ANY] + [VMEM] * len(bases),
            shape(token_count, local_feats),
            [scratch(token_count, late), scratch(local_feats, late), sems(len(late))],
        )
    return stream


def solution(mesh):
    in_specs = (
        P("sp", "tp"),
        P(None, "tp"),
        P(None, "tp", None),
        P(None, "tp", None),
        P(None, "tp", None),
        P(None, "tp", None),
        P(None, "tp", None, None),
    )
    out_specs = P("sp", "tp")
    return jax.shard_map(
        per_device, mesh=mesh, in_specs=in_specs, out_specs=out_specs, check_vma=False
    )
```
